32 devices in a mesh: sp: 8 (over z, y), tp: 4 (over x, core).
Axes of the slice: x: 2, y: 2, z: 4, core: 2. Of those that a mesh axis runs over, the one named last changes fastest.
Arguments:
- queries: bfloat16 [4096, 512], P('sp', 'tp'), may hold values from -6 to 6
- key_matrix: bfloat16 [4096, 512], P('sp', 'tp'), may hold values from -6 to 6
- value_matrix: bfloat16 [4096, 1024], P('sp', 'tp'), may hold values from -6 to 6
- channel_decay_input: bfloat16 [4096, 512], P('sp', 'tp')
- head_decay_offset: float32 [4096, 8], P('sp', 'tp'), may hold values from -1 to 0
- output_gate_input: bfloat16 [4096, 1024], P('sp', 'tp'), may hold values from -6 to 6
- head_norm_gain: float32 [128], replicated, may hold values from 0.1 to 1.9
- residual: bfloat16 [4096, 2048], P(('sp', 'tp')), may hold values from -6 to 6
- mixer_output_weight: bfloat16 [1024, 2048], replicated, may hold values from -0.1875 to 0.1875
- expert_norm_gain: float32 [2048], replicated, may hold values from 0.1 to 1.9
- routes: int32 [4096, 4], P(('sp', 'tp')), may hold values from 0 to 63, all different within a row; in each aligned block of 128 rows (0 to 127, 128 to 255, ...) at most 16 rows name the same one
- chosen_router_scores: float32 [4096, 4], P(('sp', 'tp')), may hold values from 0.1 to 1
- routed_gate_weight: bfloat16 [64, 2048, 512], P(('sp', 'tp')), may hold values from -0.125 to 0.125
- routed_up_weight: bfloat16 [64, 2048, 512], P(('sp', 'tp')), may hold values from -0.125 to 0.125
- routed_down_weight: bfloat16 [64, 512, 2048], P(('sp', 'tp')), may hold values from -0.25 to 0.25
- common_gate_weight: bfloat16 [2048, 512], replicated, may hold values from -0.125 to 0.125
- common_up_weight: bfloat16 [2048, 512], replicated, may hold values from -0.125 to 0.125
- common_down_weight: bfloat16 [512, 2048], replicated, may hold values from -0.25 to 0.25
Outputs:
- layer_out: bfloat16 [4096, 2048], P(('sp', 'tp'))
The draws below stay inside these ranges and needn't reach their ends.
Inputs may be any that keep to these rules, and one draw needn't show every extreme that they name: `routes`: each row names 4 different experts. In each aligned block of 128 rows (the rows of one device) no expert is named by more than 16 rows, a bound that some block reaches.
All inputs are finite; a program needn't handle non-finite values.
Results may differ from the reference program's by a relative error of at most 0.017.
Values may be sent and summed in bfloat16 or wider, within the bound.
A program may use at most 128 MiB of HBM per device.

```python
import math
import jax
import jax.numpy as jnp
import numpy as np
from jax import lax

D = 2048
HEADS = 8
KEY_CHANNELS = 64
VDIM = 128
BLOCK = 64
FFE = 512
SFF = 512
TOP_K = 4
TOK_DEV = 128
KW = 512
VW = 1024
TOK_SP = 512
TOKENS = 4096
EXPERTS = 64
CAP = 16


def draw_channel_decay_input(key, part):
    head_key = jax.random.fold_in(key, 11)
    channel_key = jax.random.fold_in(key, 12)
    shift_key = jax.random.fold_in(key, 13)
    jitter_key = jax.random.fold_in(key, 14)
    slow_heads = jax.random.bernoulli(head_key, 0.5, (HEADS,))
    jitter = jnp.clip(0.5 * jax.random.normal(jitter_key, (TOKENS, HEADS * KEY_CHANNELS), jnp.float32), -1.5, 1.5)
    head_base = jnp.where(slow_heads, math.log(TOKENS) - 1.5, 0.5).astype(jnp.float32)
    channel = jax.random.uniform(channel_key, (HEADS, KEY_CHANNELS), jnp.float32, -0.5, 0.5)
    column = (head_base[:, None] + channel).reshape(HEADS * KEY_CHANNELS)
    shifts = jax.random.uniform(shift_key, (TOKENS // TOK_SP,), jnp.float32, 0.0, math.log(4.0))
    rows_shift = jnp.repeat(shifts, TOK_SP)
    return (column[None, :] + jitter - rows_shift[:, None]).astype(jnp.bfloat16)


def draw_head_decay_offset(key, part):
    place_key = jax.random.fold_in(key, 21)
    size_key = jax.random.fold_in(key, 22)
    places = jax.random.randint(place_key, (3, HEADS), 0, TOKENS)
    drops = jax.random.uniform(size_key, (3, HEADS), jnp.float32, math.log(0.5), math.log(0.8))
    positions = jnp.arange(TOKENS, dtype=jnp.int32)
    landed = positions[:, None, None] == places[None, :, :]
    return jnp.sum(jnp.where(landed, drops[None, :, :], 0.0), axis=1).astype(jnp.float32)


def level_of(own_key, shape, shards, low, high):
    def one(position, blocks):
        heights = jax.random.uniform(jax.random.fold_in(jax.random.fold_in(own_key, 6), position), (blocks,), jnp.float32, low / len(shards), high / len(shards))
        return jnp.repeat(jnp.exp(heights), shape[position] // blocks).reshape((-1,) + (1,) * (len(shape) - position - 1))

    loudness = one(*shards[0])
    for cut in shards[1:]:
        loudness = loudness * one(*cut)
    return loudness


def routed_block(stream_key, own, number, rows, number_of, top, reach, skew):
    order = jax.random.permutation(stream_key, number_of)
    heavy_load, ordinary = portions_of(number_of, rows * top, reach, skew, True), portions_of(number_of, rows * top, reach, skew, False)
    places = jnp.arange(number_of)

    def named(sizes, offset_by):
        used = int((sizes > 0).sum())
        fixed = max(1, used // 4)
        passed = fixed + (places - fixed + offset_by * (used - fixed)) % max(1, number_of - fixed)
        return jnp.zeros((number_of,), jnp.int32).at[order[jnp.where(places < fixed, places, passed)]].set(jnp.asarray(sizes, jnp.int32))

    sizes = jnp.where(number % 4 == 0, named(heavy_load, number // 4), named(ordinary, number - number // 4 - 1))
    mixed = jax.random.permutation(jax.random.fold_in(own, 3), number_of)
    giver, taker = mixed[0:number_of // 2 * 2:2], mixed[1:number_of // 2 * 2:2]
    margin = jnp.minimum(sizes[giver] - 1, reach - sizes[taker]) // 2
    margin = jnp.where((giver == order[0]) | (taker == order[0]) | (sizes[taker] == 0), 0, jnp.maximum(margin, 0))
    passed = jax.random.randint(jax.random.fold_in(own, 4), (number_of // 2,), 0, 1 << 20) % (margin + 1)
    sizes = sizes.at[giver].add(-passed).at[taker].add(passed)
    items = jnp.searchsorted(jnp.cumsum(sizes), jnp.arange(rows * top), side="right").astype(jnp.int32)
    listing = items.reshape(top, rows).T
    listing = listing[jax.random.permutation(jax.random.fold_in(own, 1), rows)]
    offset_by = jax.random.randint(jax.random.fold_in(own, 2), (rows, 1), 0, top)
    return jnp.take_along_axis(listing, (jnp.arange(top)[None, :] + offset_by) % top, axis=1)


def portions_of(amount, total, reach, skew, full):
    portions = [(1 << 20) // math.isqrt(grade ** skew) + 1 for grade in range(1, amount + 1)]
    largest = reach if full else min(reach, max(-(-total // amount), total * portions[0] // sum(portions)))
    least = 1 if total - largest >= amount - 1 else 0
    given, surplus = [largest] + [least] * (amount - 1), total - largest - least * (amount - 1)
    while surplus > 0:
        movable = [i for i in range(1, amount) if given[i] < largest] or [i for i in range(1, amount) if given[i] < reach]
        mass, budget = sum([portions[i] for i in movable]), surplus
        for i in movable:
            extra = min(reach - given[i], max(1, budget * portions[i] // mass), surplus)
            given[i] = given[i] + extra
            surplus = surplus - extra
    return np.array(given)


def scatter_about(own_key, shape, deviation, reach, cuts=(), held_as=jnp.bfloat16):
    values = jax.random.normal(own_key, shape, jnp.float32) * deviation
    if len(cuts) > 0:
        values = level_of(own_key, shape, cuts, -0.22, 0.18) * values
    return jnp.clip(values, min=-reach, max=reach).astype(held_as)


def setup_inputs(seed: int = 0) -> dict:
    arg_keys = jax.random.split(jax.random.key(seed), 19)
    queries = scatter_about(arg_keys[0], (TOKENS, KW), 1.0, 6.0, ((0, 8), (1, 4)))
    key_matrix = scatter_about(arg_keys[1], (TOKENS, KW), 1.0, 6.0, ((0, 8), (1, 4)))
    value_matrix = scatter_about(arg_keys[2], (TOKENS, VW), 1.0, 6.0, ((0, 8), (1, 4)))
    channel_decay_input = draw_channel_decay_input(jax.random.fold_in(arg_keys[18], 71), 0)
    head_decay_offset = draw_head_decay_offset(jax.random.fold_in(arg_keys[18], 71), 0)
    output_gate_input = scatter_about(arg_keys[5], (TOKENS, VW), 1.0, 6.0, ((0, 8), (1, 4)))
    head_norm_gain = jnp.clip(1.0 + 0.18 * jax.random.normal(arg_keys[6], (VDIM,), jnp.float32), 0.1, 1.9)
    residual = scatter_about(arg_keys[7], (TOKENS, D), 1.0, 6.0, ((0, 32),))
    mixer_output_weight = scatter_about(arg_keys[8], (VW, D), VW ** -0.5, 0.1875)
    expert_norm_gain = jnp.clip(1.0 + 0.18 * jax.random.normal(arg_keys[9], (D,), jnp.float32), 0.1, 1.9)
    routes_keys = jax.random.split(jax.random.fold_in(arg_keys[10], 1), TOKENS // TOK_DEV)
    routes_turns = jax.random.permutation(jax.random.fold_in(arg_keys[10], 3), TOKENS // TOK_DEV)
    routes = jax.vmap(lambda own, number: routed_block(jax.random.fold_in(arg_keys[10], 2), own, number, TOK_DEV, EXPERTS, TOP_K, CAP, 2))(routes_keys, routes_turns).reshape((TOKENS, TOP_K))
    chosen_router_scores = jnp.clip(jnp.exp(math.log(1.0) - 2.3025851 * jax.random.uniform(arg_keys[11], (TOKENS, TOP_K), jnp.float32) ** level_of(arg_keys[11], (TOKENS, TOP_K), ((0, 32),), -0.2, 0.2)), 0.1, 1.0)
    routed_gate_weight = scatter_about(arg_keys[12], (EXPERTS, D, FFE), D ** -0.5, 0.125, ((0, 32),))
    routed_up_weight = scatter_about(arg_keys[13], (EXPERTS, D, FFE), D ** -0.5, 0.125, ((0, 32),))
    routed_down_weight = scatter_about(arg_keys[14], (EXPERTS, FFE, D), FFE ** -0.5, 0.25, ((0, 32),))
    common_gate_weight = scatter_about(arg_keys[15], (D, SFF), D ** -0.5, 0.125)
    common_up_weight = scatter_about(arg_keys[16], (D, SFF), D ** -0.5, 0.125)
    common_down_weight = scatter_about(arg_keys[17], (SFF, D), SFF ** -0.5, 0.25)
    return dict(queries=queries, key_matrix=key_matrix, value_matrix=value_matrix, channel_decay_input=channel_decay_input, head_decay_offset=head_decay_offset, output_gate_input=output_gate_input, head_norm_gain=head_norm_gain, residual=residual, mixer_output_weight=mixer_output_weight, expert_norm_gain=expert_norm_gain, routes=routes, chosen_router_scores=chosen_router_scores, routed_gate_weight=routed_gate_weight, routed_up_weight=routed_up_weight, routed_down_weight=routed_down_weight, common_gate_weight=common_gate_weight, common_up_weight=common_up_weight, common_down_weight=common_down_weight)


eps_norm = 1e-06
decay_running = 16.0
routed_scale = 2.5

def split_heads(values, columns):
    blocks = values.shape[0] // BLOCK
    return values.astype(jnp.float32).reshape(blocks, BLOCK, HEADS, columns).transpose(2, 0, 1, 3)

def recurrent_mixer(queries, key_matrix, value_matrix, channel_decay_input, head_decay_offset, output_gate_input, head_norm_gain):
    decay_spike_columns = jnp.repeat(head_decay_offset, KEY_CHANNELS, axis=1)
    decay_logarithm = jax.nn.log_sigmoid(channel_decay_input.astype(jnp.float32)) / decay_running + decay_spike_columns
    within = jnp.cumsum(split_heads(decay_logarithm, KEY_CHANNELS), axis=2)
    block_end = within[:, :, -1:, :]
    q_heads = split_heads(queries, KEY_CHANNELS) * KEY_CHANNELS ** (-0.5)
    k_heads = split_heads(key_matrix, KEY_CHANNELS)
    v_heads = split_heads(value_matrix, VDIM)
    q_decay = q_heads * jnp.exp(within)
    k_grow = k_heads * jnp.exp(-within)
    k_tail = k_heads * jnp.exp(block_end - within)
    causal = jnp.tril(jnp.ones((BLOCK, BLOCK), dtype=bool))
    scores = jnp.where(causal, jnp.einsum('hnid,hnjd->hnij', q_decay, k_grow), 0.0)
    output = jnp.einsum('hnij,hnje->hnie', scores, v_heads)
    block_state = jnp.einsum('hncd,hnce->nhde', k_tail, v_heads)
    block_decay = jnp.moveaxis(jnp.exp(block_end[:, :, 0, :]), 1, 0)

    def advance(carried, block_inputs):
        added_state, factor = block_inputs
        return (factor[..., None] * carried + added_state, carried)
    start_state = jnp.zeros((HEADS, KEY_CHANNELS, VDIM), jnp.float32)
    _, entering = lax.scan(advance, start_state, (block_state, block_decay))
    output = output + jnp.einsum('hncd,nhde->hnce', q_decay, entering)
    output = output.transpose(1, 2, 0, 3).reshape(-1, HEADS, VDIM)
    inv_rms = lax.rsqrt(lax.optimization_barrier(jnp.mean(output * output, axis=-1, keepdims=True)) + eps_norm)
    normed = (output * inv_rms * head_norm_gain).reshape(-1, HEADS * VDIM)
    return (normed * jax.nn.silu(output_gate_input.astype(jnp.float32))).astype(jnp.bfloat16)

def expert_block(picked_rows, gate_weight, up_weight, down_weight):
    gate_pre = jnp.dot(picked_rows, gate_weight, preferred_element_type=jnp.float32)
    up_pre = jnp.dot(picked_rows, up_weight, preferred_element_type=jnp.float32)
    hidden = (jax.nn.silu(gate_pre) * up_pre).astype(jnp.bfloat16)
    return jnp.dot(hidden, down_weight, preferred_element_type=jnp.float32)

def reference(queries, key_matrix, value_matrix, channel_decay_input, head_decay_offset, output_gate_input, head_norm_gain, residual, mixer_output_weight, expert_norm_gain, routes, chosen_router_scores, routed_gate_weight, routed_up_weight, routed_down_weight, common_gate_weight, common_up_weight, common_down_weight):
    gated_output = recurrent_mixer(queries, key_matrix, value_matrix, channel_decay_input, head_decay_offset, output_gate_input, head_norm_gain)
    middle = (residual.astype(jnp.float32) + jnp.dot(gated_output, mixer_output_weight, preferred_element_type=jnp.float32)).astype(jnp.bfloat16)
    middle_wide = middle.astype(jnp.float32)
    inv_rms = lax.rsqrt(lax.optimization_barrier(jnp.mean(middle_wide * middle_wide, axis=-1, keepdims=True)) + eps_norm)
    normed = (middle_wide * inv_rms * expert_norm_gain).astype(jnp.bfloat16)
    weights = routed_scale * chosen_router_scores / lax.optimization_barrier(jnp.sum(chosen_router_scores, axis=-1, keepdims=True))
    flat_expert = routes.reshape(-1).astype(jnp.int32)
    assigned = TOKENS * TOP_K
    flat_token = (jnp.arange(assigned, dtype=jnp.int32) // TOP_K).astype(jnp.int32)
    flat_weight = weights.reshape(-1)
    sorted_ids = jnp.argsort(flat_expert, stable=True).astype(jnp.int32)
    counts = jnp.bincount(flat_expert, length=EXPERTS).astype(jnp.int32)
    starts = (jnp.cumsum(counts) - counts).astype(jnp.int32)
    slot_room = TOKENS // TOK_DEV * CAP
    order_pad = jnp.concatenate([sorted_ids, jnp.full((slot_room,), assigned, jnp.int32)])
    token_pad = jnp.concatenate([flat_token, jnp.full((1,), TOKENS, jnp.int32)])
    weight_pad = jnp.concatenate([flat_weight, jnp.zeros((1,), jnp.float32)])
    normed_pad = jnp.concatenate([normed, jnp.zeros((1, D), jnp.bfloat16)], axis=0)

    def one_expert(summed, expert_id):
        picked = lax.dynamic_slice_in_dim(order_pad, starts[expert_id], slot_room)
        live_slot = jnp.arange(slot_room, dtype=jnp.int32) < counts[expert_id]
        picked = jnp.where(live_slot, picked, assigned).astype(jnp.int32)
        tokens = token_pad[picked]
        picked_rows = normed_pad[tokens]
        result = expert_block(picked_rows, routed_gate_weight[expert_id], routed_up_weight[expert_id], routed_down_weight[expert_id]).astype(jnp.bfloat16)
        return (summed.at[tokens].add(weight_pad[picked][:, None] * result.astype(jnp.float32)), None)
    routed, _ = lax.scan(one_expert, jnp.zeros((TOKENS + 1, D), jnp.float32), jnp.arange(EXPERTS, dtype=jnp.int32))
    shared = expert_block(normed, common_gate_weight, common_up_weight, common_down_weight)
    return (middle_wide + routed[:TOKENS] + shared).astype(jnp.bfloat16)
```

```python
import functools
import math

import jax
import jax.numpy as jnp
from jax import lax
from jax.experimental import pallas as pl
from jax.experimental.pallas import tpu as pltpu
from jax.sharding import PartitionSpec as P

D = 2048
KEY_CHANNELS = 64
VDIM = 128
BLOCK = 64
TOP_K = 4


eps_norm = 1e-06
decay_running = 16.0
routed_scale = 2.5


def peer(sp, tp):
    return {"sp": sp, "tp": tp}


def greet(targets):
    barrier = pltpu.get_barrier_semaphore()
    for target in targets:
        pl.semaphore_signal(
            barrier, inc=1, device_id=target, device_id_type=pl.DeviceIdType.MESH
        )
    pl.semaphore_wait(barrier, len(targets))


def remote(src, dst, send, recv, target):
    return pltpu.make_async_remote_copy(
        src_ref=src,
        dst_ref=dst,
        send_sem=send,
        recv_sem=recv,
        device_id=target,
        device_id_type=pl.DeviceIdType.MESH,
    )


def remote_call(kernel, out_shape, operands, scratch, number, flops=1_000_000):
    multi = isinstance(out_shape, (tuple, list))
    vmem = pl.BlockSpec(memory_space=pltpu.VMEM)
    return pl.pallas_call(
        kernel,
        out_shape=out_shape,
        in_specs=[vmem] * len(operands),
        out_specs=[vmem] * len(out_shape) if multi else vmem,
        scratch_shapes=scratch,
        compiler_params=pltpu.CompilerParams(
            collective_id=number, has_side_effects=True, vmem_limit_bytes=56 * 1024 * 1024
        ),
    )(*operands)


def gather_sp_kernel(count, x_ref, y_ref, xs_ref, ys_ref, send, recv):
    me, tp = lax.axis_index("sp"), lax.axis_index("tp")
    targets = [peer(lax.rem(me + d, count), tp) for d in range(1, count)]
    greet(targets)
    copies = []
    for d in range(1, count):
        for i, (src, dst) in enumerate(((x_ref, xs_ref), (y_ref, ys_ref))):
            copies.append(
                remote(src, dst.at[me], send.at[i, d], recv.at[i, d], targets[d - 1])
            )
            copies[-1].start()
    xs_ref[me] = x_ref[...]
    ys_ref[me] = y_ref[...]
    for copy in copies:
        copy.wait()


def gather_sp(state, packet):
    count = lax.axis_size("sp")
    return remote_call(
        functools.partial(gather_sp_kernel, count),
        [
            jax.ShapeDtypeStruct((count,) + state.shape, state.dtype),
            jax.ShapeDtypeStruct((count,) + packet.shape, packet.dtype),
        ],
        [state, packet],
        [pltpu.SemaphoreType.DMA((2, count)), pltpu.SemaphoreType.DMA((2, count))],
        0,
    )


def swap_tp_kernel(count, x_ref, out_ref, send, recv):
    sp, me = lax.axis_index("sp"), lax.axis_index("tp")
    width = x_ref.shape[2]
    targets = [peer(sp, lax.rem(me + d, count)) for d in range(1, count)]
    greet(targets)
    columns = pl.ds(pl.multiple_of(me * width, width), width)
    copies = []
    for d in range(1, count):
        copies.append(
            remote(
                x_ref.at[lax.rem(me + d, count)],
                out_ref.at[:, columns],
                send.at[d],
                recv.at[d],
                targets[d - 1],
            )
        )
        copies[-1].start()
    out_ref[:, columns] = x_ref[me]
    for copy in copies:
        copy.wait()


def swap_tp(stacked):
    count = lax.axis_size("tp")
    return remote_call(
        functools.partial(swap_tp_kernel, count),
        jax.ShapeDtypeStruct((stacked.shape[1], count * stacked.shape[2]), stacked.dtype),
        [stacked],
        [pltpu.SemaphoreType.DMA((count,)), pltpu.SemaphoreType.DMA((count,))],
        1,
    )


class Place:
    def __init__(self, sp_size, tp_size):
        self.deep = math.gcd(sp_size, 4)
        self.rows = sp_size // self.deep
        self.tp_size = tp_size
        self.flat = self.rows * tp_size

    def here(self):
        sp, tp = lax.axis_index("sp"), lax.axis_index("tp")
        self.sp, self.tp = sp, tp
        self.a = sp // self.rows
        self.b = lax.rem(sp, self.rows)
        self.p = self.b * self.tp_size + tp
        return self

    def column(self, a):
        return peer(a * self.rows + self.b, self.tp)

    def plane(self, p):
        return peer(self.a * self.rows + p // self.tp_size, lax.rem(p, self.tp_size))

    def across(self, q):
        return lax.rem(self.p + q, self.flat)

    def nearest(self, i):
        last = self.deep - 1
        span = jnp.minimum(self.a, last - self.a)
        zigzag = self.a + ((i + 1) // 2 if i % 2 else -(i // 2))
        return jnp.where(i <= 2 * span, zigzag, jnp.where(self.a < last - self.a, i, last - i))


def tiles_of(width, most=512):
    step = math.gcd(width, most)
    return [slice(i, i + step) for i in range(0, width, step)]


def flatten_rows(block):
    groups, rows, width = block.shape
    if rows % 16 == 0:
        return block.reshape(groups * rows, width)
    return block.astype(jnp.float32).reshape(groups * rows, width).astype(jnp.bfloat16)


def experts_kernel(
    sizes, x_ref, middle_ref, select_ref, mix_ref, gate_ref, up_ref, down_ref,
    wide_gate, wide_up, wide_down, out_ref,
    column_ref, stage_ref, arrived_ref, made_ref, back_ref, sent_ref, came_ref, base_ref,
    hidden_ref, own_gate, own_up, own_down,
    weight_sem, zs, zr, ps, pr, bs, br, ss, sr,
):
    at = Place(*sizes).here()
    last = at.deep - 1
    flat, rows = stage_ref.shape[1], stage_ref.shape[2]
    width = x_ref.shape[1]
    experts = own_gate.shape[0]
    cap = rows // experts
    loads = [
        pltpu.make_async_copy(wide_gate, own_gate, weight_sem.at[0]),
        pltpu.make_async_copy(wide_up, own_up, weight_sem.at[1]),
        pltpu.make_async_copy(wide_down, own_down, weight_sem.at[2]),
    ]
    for load in loads:
        load.start()
    has_right, has_left = at.a < last, at.a > 0
    greet(
        [at.column(lax.rem(at.a + d, at.deep)) for d in range(1, at.deep)]
        + [at.plane(at.across(q)) for q in range(1, flat)]
    )

    def relay(source, owner, side):
        return remote(
            source,
            column_ref.at[owner],
            zs.at[side, owner],
            zr.at[owner],
            at.column(at.a + (1 if side == 0 else -1)),
        )

    def sends(owner):
        right = has_right & (owner <= at.a)
        left = has_left & (owner >= at.a)
        return right, left

    def forward(source, owner):
        right, left = sends(owner)
        pl.when(right)(lambda: relay(source, owner, 0).start())
        pl.when(left)(lambda: relay(source, owner, 1).start())

    def out_copy(owner, q):
        target = at.across(q)
        return remote(
            stage_ref.at[owner, target],
            arrived_ref.at[owner, at.p],
            ps.at[owner, q],
            pr.at[owner, q],
            at.plane(target),
        )

    def back_copy(owner, q):
        target = at.across(q)
        return remote(
            made_ref.at[owner, target],
            back_ref.at[owner, at.p],
            bs.at[owner, q],
            br.at[owner, q],
            at.plane(target),
        )

    def pass_on(owner, source):
        for cut in tiles_of(width):
            picked = jnp.dot(
                select_ref[owner], source[:, cut], preferred_element_type=jnp.float32
            )
            stage_ref[owner, :, :, cut] = picked.reshape(flat, rows, -1).astype(jnp.bfloat16)
        for q in range(1, flat):
            out_copy(owner, q).start()
        arrived_ref[owner, at.p] = stage_ref[owner, at.p]

    def run_experts(owner):
        for q in range(1, flat):
            out_copy(owner, q).wait_recv()
        for e in range(experts):
            mine = slice(e * cap, (e + 1) * cap)
            for cut in tiles_of(own_gate.shape[2], 256):
                block = flatten_rows(arrived_ref[owner, :, mine, :])
                gate = jnp.dot(block, own_gate[e, :, cut], preferred_element_type=jnp.float32)
                up = jnp.dot(block, own_up[e, :, cut], preferred_element_type=jnp.float32)
                hidden_ref[:, cut] = (jax.nn.silu(gate) * up).astype(jnp.bfloat16)
            for cut in tiles_of(width):
                down = jnp.dot(
                    hidden_ref[...], own_down[e, :, cut], preferred_element_type=jnp.float32
                )
                made_ref[owner, :, mine, cut] = down.reshape(flat, cap, -1).astype(jnp.bfloat16)
        for q in range(1, flat):
            back_copy(owner, q).start()
        back_ref[owner, at.p] = made_ref[owner, at.p]

    order = [at.nearest(i) for i in range(at.deep)]
    forward(x_ref, at.a)
    pass_on(at.a, x_ref)
    tokens = x_ref.shape[0]
    for cut in tiles_of(gate_ref.shape[1], 256):
        gate = jnp.dot(x_ref[...], gate_ref[:, cut], preferred_element_type=jnp.float32)
        up = jnp.dot(x_ref[...], up_ref[:, cut], preferred_element_type=jnp.float32)
        sent_ref[at.a, :, cut] = (jax.nn.silu(gate) * up).astype(jnp.bfloat16)
    for cut in tiles_of(width):
        base_ref[:, cut] = middle_ref[:, cut].astype(jnp.float32) + jnp.dot(
            sent_ref[at.a, :, : gate_ref.shape[1]],
            down_ref[:, cut],
            preferred_element_type=jnp.float32,
        )
    for i in range(1, at.deep + 1):
        if i < at.deep:
            relay(x_ref, order[i], 0).wait_recv()
            forward(column_ref.at[order[i]], order[i])
            pass_on(order[i], column_ref.at[order[i]])
        if i == 1:
            for load in loads:
                load.wait()
        run_experts(order[i - 1])

    def gather_back(owner):
        for q in range(1, flat):
            back_copy(owner, q).wait_recv()

    def mixed(owner, cut):
        block = flatten_rows(back_ref[owner, :, :, cut])
        return jnp.dot(mix_ref[owner], block, preferred_element_type=jnp.float32)

    def toward(owner, side):
        return remote(
            sent_ref.at[owner],
            came_ref.at[side, owner],
            ss.at[owner],
            sr.at[side, owner],
            at.column(at.a + (-1 if side == 0 else 1)),
        )

    def step(owner, side, more):
        for cut in tiles_of(width):
            part = mixed(owner, cut)
            if more:
                part = part + came_ref[side, owner, :, cut].astype(jnp.float32)
            sent_ref[owner, :, cut] = part.astype(jnp.bfloat16)
        toward(owner, side).start()

    for i in range(at.deep - 1, 0, -1):
        owner = order[i]
        gather_back(owner)
        for side, goes, far in ((0, owner < at.a, has_right), (1, owner > at.a, has_left)):

            @pl.when(goes & far)
            def _(owner=owner, side=side):
                toward(owner, side).wait_recv()
                step(owner, side, True)

            @pl.when(goes & jnp.logical_not(far))
            def _(owner=owner, side=side):
                step(owner, side, False)

    gather_back(at.a)
    for cut in tiles_of(width):
        base_ref[:, cut] += mixed(at.a, cut)
    for side, far in ((0, has_right), (1, has_left)):

        @pl.when(far)
        def _(side=side):
            toward(at.a, side).wait_recv()
            for cut in tiles_of(width):
                base_ref[:, cut] += came_ref[side, at.a, :, cut].astype(jnp.float32)

    out_ref[...] = base_ref[...].astype(out_ref.dtype)
    for i in range(at.deep):
        owner = order[i]
        right, left = sends(owner)
        pl.when(right)(lambda owner=owner: relay(x_ref, owner, 0).wait_send())
        pl.when(left)(lambda owner=owner: relay(x_ref, owner, 1).wait_send())
        for q in range(1, flat):
            out_copy(owner, q).wait_send()
            back_copy(owner, q).wait_send()
        if i > 0:
            toward(owner, 0).wait_send()


def experts_layer(normed, middle, select, mix, common, routed):
    sizes = (lax.axis_size("sp"), lax.axis_size("tp"))
    at = Place(*sizes)
    tokens, width = normed.shape
    slots = select.shape[1]
    box = (at.deep, at.flat, slots // at.flat, width)
    chunk = (at.deep, tokens, width)
    dma = pltpu.SemaphoreType.DMA
    half = jnp.bfloat16
    vmem = pl.BlockSpec(memory_space=pltpu.VMEM)
    far = pl.BlockSpec(memory_space=pl.ANY)
    experts = routed[0].shape[0]
    return pl.pallas_call(
        functools.partial(experts_kernel, sizes),
        out_shape=jax.ShapeDtypeStruct((tokens, width), half),
        in_specs=[vmem] * 7 + [far] * 3,
        out_specs=vmem,
        scratch_shapes=[
            pltpu.VMEM(chunk, half),
            pltpu.VMEM(box, half),
            pltpu.VMEM(box, half),
            pltpu.VMEM(box, half),
            pltpu.VMEM(box, half),
            pltpu.VMEM(chunk, half),
            pltpu.VMEM((2,) + chunk, half),
            pltpu.VMEM((tokens, width), jnp.float32),
            pltpu.VMEM((slots // experts, routed[0].shape[2]), half),
            pltpu.VMEM(routed[0].shape, half),
            pltpu.VMEM(routed[1].shape, half),
            pltpu.VMEM(routed[2].shape, half),
            dma((3,)),
            dma((2, at.deep)),
            dma((at.deep,)),
            dma((at.deep, at.flat)),
            dma((at.deep, at.flat)),
            dma((at.deep, at.flat)),
            dma((at.deep, at.flat)),
            dma((at.deep,)),
            dma((2, at.deep)),
        ],
        compiler_params=pltpu.CompilerParams(
            collective_id=2, has_side_effects=True, vmem_limit_bytes=60 * 1024 * 1024
        ),
    )(normed, middle, select, mix, *common, *routed)


def on_device(
    queries,
    key_matrix,
    value_matrix,
    channel_decay_input,
    head_decay_offset,
    output_gate_input,
    head_norm_gain,
    residual,
    mixer_output_weight,
    expert_norm_gain,
    routes,
    chosen_router_scores,
    routed_gate_weight,
    routed_up_weight,
    routed_down_weight,
    common_gate_weight,
    common_up_weight,
    common_down_weight,
):
    device_heads = head_decay_offset.shape[1]
    seq_rows = queries.shape[0]
    blocks = seq_rows // BLOCK

    def split_local(values, columns):
        return (
            values.astype(jnp.float32)
            .reshape(blocks, BLOCK, device_heads, columns)
            .transpose(2, 0, 1, 3)
        )

    decay_spike_columns = jnp.repeat(head_decay_offset, KEY_CHANNELS, axis=1)
    decay_logarithm = (
        jax.nn.log_sigmoid(channel_decay_input.astype(jnp.float32)) / decay_running
        + decay_spike_columns
    )
    within = jnp.einsum(
        "ij,hnjd->hnid",
        jnp.tril(jnp.ones((BLOCK, BLOCK), jnp.float32)),
        split_local(decay_logarithm, KEY_CHANNELS),
        precision=lax.Precision.HIGHEST,
    )
    block_end = within[:, :, -1, :]
    q_heads = split_local(queries, KEY_CHANNELS) * KEY_CHANNELS ** (-0.5)
    k_heads = split_local(key_matrix, KEY_CHANNELS)
    v_heads = split_local(value_matrix, VDIM)
    q_decay = q_heads * jnp.exp(within)
    k_grow = k_heads * jnp.exp(-within)
    k_tail = k_heads * jnp.exp(block_end[:, :, None, :] - within)
    causal = jnp.tril(jnp.ones((BLOCK, BLOCK), dtype=bool))
    scores = jnp.where(causal, jnp.einsum("hnid,hnjd->hnij", q_decay, k_grow), 0.0)
    inside = jnp.einsum("hnij,hnje->hnie", scores, v_heads)
    block_state = jnp.einsum("hncd,hnce->hnde", k_tail, v_heads)
    inclusive = jnp.cumsum(block_end, axis=1)
    exclusive = inclusive - block_end
    before = jnp.arange(blocks)[:, None] > jnp.arange(blocks)[None, :]
    spread = jnp.exp(
        jnp.where(
            before[None, :, :, None], exclusive[:, :, None, :] - inclusive[:, None, :, :], -jnp.inf
        )
    )
    local_start = jnp.einsum("hnmd,hmde->hnde", spread, block_state)
    total_log = inclusive[:, -1, :]
    tail_weight = jnp.exp(total_log[:, None, :] - inclusive)
    device_state = jnp.einsum("hnd,hnde->hde", tail_weight, block_state)
    lanes = VDIM
    tok_count = residual.shape[0]
    sp_index = lax.axis_index("sp")
    sp_size = lax.axis_size("sp")
    state_rows = device_heads * KEY_CHANNELS
    parts = [
        total_log.reshape(-1, lanes),
        routes.T.astype(jnp.float32).reshape(-1, lanes),
        chosen_router_scores.T.reshape(-1, lanes),
    ]
    stops = [sum(part.shape[0] for part in parts[: i + 1]) for i in range(len(parts))]
    spare = -stops[-1] % 8
    packet = jnp.concatenate(parts + [jnp.zeros((spare, lanes), jnp.float32)], axis=0)
    state = device_state.reshape(state_rows, lanes).astype(jnp.bfloat16)
    states, gathered = gather_sp(state, packet)
    states = states.reshape(sp_size, device_heads, KEY_CHANNELS, VDIM).astype(jnp.float32)
    logs = gathered[:, : stops[0]].reshape(sp_size, device_heads, KEY_CHANNELS)
    ahead = (jnp.arange(sp_size) < sp_index)[:, None, None]
    logs = jnp.where(ahead, logs, 0.0)
    later = (jnp.arange(sp_size)[:, None] < jnp.arange(sp_size)[None, :])[:, :, None, None]
    after = jnp.sum(jnp.where(later, logs[None], 0.0), axis=1)
    reach = jnp.where(ahead, jnp.exp(after), 0.0)
    carried = jnp.sum(reach[..., None] * states, axis=0)
    entering = local_start + jnp.exp(exclusive)[..., None] * carried[:, None, :, :]
    output = inside + jnp.einsum("hncd,hnde->hnce", q_decay, entering)
    output = output.transpose(1, 2, 0, 3).reshape(seq_rows, device_heads, VDIM)
    inv_rms = lax.rsqrt(jnp.mean(output * output, axis=-1, keepdims=True) + eps_norm)
    normed_heads = (output * inv_rms * head_norm_gain).reshape(seq_rows, device_heads * VDIM)
    gated_output = (normed_heads * jax.nn.silu(output_gate_input.astype(jnp.float32))).astype(
        jnp.bfloat16
    )
    stacked = gated_output.reshape(lax.axis_size("tp"), tok_count, gated_output.shape[1])
    projected = jnp.dot(
        swap_tp(stacked), mixer_output_weight, preferred_element_type=jnp.float32
    )
    middle = (residual.astype(jnp.float32) + projected).astype(jnp.bfloat16)
    middle_wide = middle.astype(jnp.float32)
    norm_scale = lax.rsqrt(jnp.mean(middle_wide * middle_wide, axis=-1, keepdims=True) + eps_norm)
    normed = (middle_wide * norm_scale * expert_norm_gain).astype(jnp.bfloat16)
    devices = sp_size * lax.axis_size("tp")
    exp_dev = routed_gate_weight.shape[0]
    cap_slots = 2 * TOP_K * tok_count // (exp_dev * devices)
    at = Place(sp_size, lax.axis_size("tp")).here()
    column = lax.dynamic_index_in_dim(
        gathered.reshape(at.deep, at.rows, -1, lanes), at.b, 1, False
    )
    names = column[:, stops[0] : stops[1]].reshape(at.deep, TOP_K, 1, tok_count)
    scores_all = column[:, stops[1] : stops[2]].reshape(at.deep, TOP_K, 1, tok_count)
    weights = routed_scale * scores_all / jnp.sum(scores_all, axis=1, keepdims=True)
    plane_experts = at.flat * exp_dev
    expert = (at.a * plane_experts + jnp.arange(plane_experts)).astype(jnp.float32)
    hit = (names == expert[None, None, :, None]).astype(jnp.float32)
    chosen = jnp.sum(hit, axis=1)
    weight_of = jnp.sum(hit * weights, axis=1)
    sooner = jnp.triu(jnp.ones((tok_count, tok_count), jnp.bfloat16), 1)
    rank = jnp.einsum(
        "aeu,ut->aet",
        chosen.astype(jnp.bfloat16),
        sooner,
        preferred_element_type=jnp.float32,
    )
    slot = jnp.arange(cap_slots, dtype=jnp.float32)[None, None, :, None]
    taken = (rank[:, :, None, :] == slot) & (chosen[:, :, None, :] > 0.0)
    slots = plane_experts * cap_slots
    select = taken.astype(jnp.bfloat16).reshape(at.deep, slots, tok_count)
    mix = jnp.where(taken, weight_of[:, :, None, :], 0.0).astype(jnp.bfloat16)
    mix = mix.reshape(at.deep, slots, tok_count).transpose(0, 2, 1)
    return experts_layer(
        normed,
        middle,
        select,
        mix,
        (common_gate_weight, common_up_weight, common_down_weight),
        (routed_gate_weight, routed_up_weight, routed_down_weight),
    )


def solution(mesh):
    placed = (
        P("sp", "tp"),
        P("sp", "tp"),
        P("sp", "tp"),
        P("sp", "tp"),
        P("sp", "tp"),
        P("sp", "tp"),
        P(),
        P(("sp", "tp"), None),
        P(),
        P(),
        P(("sp", "tp"), None),
        P(("sp", "tp"), None),
        P(("sp", "tp"), None, None),
        P(("sp", "tp"), None, None),
        P(("sp", "tp"), None, None),
        P(),
        P(),
        P(),
    )
    return jax.shard_map(
        on_device, mesh=mesh, in_specs=placed, out_specs=P(("sp", "tp"), None), check_vma=False
    )
```
